32 devices in a mesh: dp: 4 (over y, x), kv: 4 (over z), tp: 2 (over core).
Axes of the slice: x: 2, y: 2, z: 4, core: 2. Of those that a mesh axis runs over, the one named last changes fastest.
Arguments:
- tokens: bfloat16 [16, 4096], P('dp', ('kv', 'tp')), parts along dimension 0, may hold values from -6 to 6
- mix_gain: float32 [4096], replicated, may hold values from 0.1 to 1.9
- w_query: bfloat16 [4096, 2048], P('kv', 'tp'), may hold values from -0.09375 to 0.09375
- w_key: bfloat16 [4096, 2048], P('kv', 'tp'), may hold values from -0.09375 to 0.09375
- w_value: bfloat16 [4096, 4096], P('kv', 'tp'), may hold values from -0.09375 to 0.09375
- w_igate: bfloat16 [4096, 16], replicated, may hold values from -0.09375 to 0.09375
- w_fgate: bfloat16 [4096, 16], replicated, may hold values from -0.09375 to 0.09375
- igate_bias: float32 [16], replicated, may hold values from -3 to 1
- fgate_bias: float32 [16], replicated, may hold values from -2 to 5
- memory: float32 [16, 16, 256, 128], P(('dp', 'kv'), 'tp'), parts along dimension 0, may hold values from -6 to 6
- normalizer: float32 [16, 16, 128], P(('dp', 'kv'), 'tp'), parts along dimension 0, may hold values from -6 to 6
- stabilizer: float32 [16, 16], P(('dp', 'kv'), 'tp'), parts along dimension 0, may hold values from -3 to 3
- w_output: bfloat16 [4096, 4096], P('tp', 'kv'), may hold values from -0.09375 to 0.09375
- mlp_gain: float32 [4096], replicated, may hold values from 0.1 to 1.9
- w_up: bfloat16 [4096, 16384], P(None, ('kv', 'tp')), may hold values from -0.09375 to 0.09375
- w_down: bfloat16 [16384, 4096], P(('kv', 'tp')), may hold values from -0.0625 to 0.0625
Outputs:
- new_tokens: bfloat16 [16, 4096], P('dp', ('kv', 'tp')), parts along dimension 0
- new_memory: float32 [16, 16, 256, 128], P(('dp', 'kv'), 'tp'), parts along dimension 0
- new_normalizer: float32 [16, 16, 128], P(('dp', 'kv'), 'tp'), parts along dimension 0
- new_stabilizer: float32 [16, 16], P(('dp', 'kv'), 'tp'), parts along dimension 0
The draws below stay inside these ranges and needn't reach their ends.
There are 4 independent parts, one for each index of `dp`. The reference program is written for one: setup_inputs(seed, part) draws one part's arguments, and reference() takes and returns one part's arrays. A program takes and returns all parts, laid end to end along the dimension named above; an argument that names none is the same for every part. Nothing has to cross between parts.
All inputs are finite; a program needn't handle non-finite values.
Results may differ from the reference program's by a relative error of at most 0.019.
Values may be sent and summed in bfloat16 or wider, within the bound.
A program may use at most 128 MiB of HBM per device.

```python
import jax
import jax.numpy as jnp
from jax import lax

D = 4096
NH = 16
DV = 256
DQK = 128
FF = 16384
BATCH = 4
N_TP = 2


def with_spikes(array, key, source, target, shards_of, factor):
    def block_of(axis_at):
        return (jnp.arange(array.shape[axis_at]) // (array.shape[axis_at] // shards_of)).reshape((-1,) + (1,) * (array.ndim - 1 - axis_at))

    near = jax.random.permutation(key, shards_of)[block_of(target)]
    far = (block_of(target) + shards_of // 2) % shards_of
    return jnp.where((block_of(source) == near) | (block_of(source) == far), factor * array, array)


def levels(stream_key, shape, split, least, high):
    level, own = 1.0, jax.random.fold_in(stream_key, 6)
    for position, parts in split:
        heights = jnp.exp(jax.random.uniform(jax.random.fold_in(own, position), (parts,), jnp.float32, least / len(split), high / len(split)))
        level = level * jnp.repeat(heights, shape[position] // parts).reshape([-1 if axis == position else 1 for axis in range(len(shape))])
    return level


def bell_draw(stream_key, dims, width, most, cuts=(), dtype=jnp.bfloat16):
    values = jax.random.normal(stream_key, dims, jnp.float32) * width
    if len(cuts) > 0:
        values = levels(stream_key, dims, cuts, -0.22, 0.18) * values
    return jnp.clip(values, min=-most, max=most).astype(dtype)


def gaussian_with(key, shape, spread, reach, cuts, heavy, dtype=jnp.bfloat16):
    drawn = spread * jax.random.normal(key, shape, jnp.float32)
    if cuts:
        drawn = drawn * levels(key, shape, cuts, -0.22, 0.18)
    return jnp.clip(with_spikes(drawn, jax.random.fold_in(key, 3), *heavy), -reach, reach).astype(dtype)


def setup_inputs(seed: int = 0, part: int = 0) -> dict:
    key_of = jax.random.split(jax.random.key(seed), 17)
    part_splits = jax.random.split(jax.random.fold_in(key_of[16], part), 17)
    tokens = gaussian_with(part_splits[0], (BATCH, D), 1.0, 6.0, ((1, 8),), (1, 0, 4, 2.0))
    mix_gain = jnp.clip(1.0 + 0.18 * jax.random.normal(key_of[1], (D,), jnp.float32), 0.1, 1.9)
    w_query = bell_draw(key_of[2], (D, NH * DQK), D ** -0.5, 0.09375, ((0, 4), (1, 2)))
    w_key = bell_draw(key_of[3], (D, NH * DQK), D ** -0.5, 0.09375, ((0, 4), (1, 2)))
    w_value = bell_draw(key_of[4], (D, NH * DV), D ** -0.5, 0.09375, ((0, 4), (1, 2)))
    w_igate = bell_draw(key_of[5], (D, NH), D ** -0.5, 0.09375)
    w_fgate = bell_draw(key_of[6], (D, NH), D ** -0.5, 0.09375)
    igate_bias = jnp.clip(jax.random.uniform(key_of[7], (NH,), jnp.float32, -3.0, 1.0), -3.0, 1.0)
    fgate_bias = jnp.clip(jax.random.uniform(key_of[8], (NH,), jnp.float32, -2.0, 5.0), -2.0, 5.0)
    memory = bell_draw(part_splits[9], (BATCH, NH, DV, DQK), 1.0, 6.0, ((0, 4), (1, 2)), jnp.float32)
    normalizer = bell_draw(part_splits[10], (BATCH, NH, DQK), 1.0, 6.0, ((0, 4), (1, 2)), jnp.float32)
    stabilizer = jnp.clip(jax.random.uniform(part_splits[11], (BATCH, NH), jnp.float32, -3.0, 3.0) * levels(part_splits[11], (BATCH, NH), ((0, 4), (1, 2)), -0.4, 0.0), -3.0, 3.0)
    w_output = bell_draw(key_of[12], (NH * DV, D), (NH * DV) ** -0.5, 0.09375, ((0, 2), (1, 4)))
    mlp_gain = jnp.clip(1.0 + 0.18 * jax.random.normal(key_of[13], (D,), jnp.float32), 0.1, 1.9)
    w_up = bell_draw(key_of[14], (D, FF), D ** -0.5, 0.09375, ((1, 8),))
    w_down = gaussian_with(key_of[15], (FF, D), FF ** -0.5, 0.0625, ((0, 8),), (0, 1, 8, 2.0))
    return {"tokens": tokens, "mix_gain": mix_gain, "w_query": w_query, "w_key": w_key, "w_value": w_value, "w_igate": w_igate, "w_fgate": w_fgate, "igate_bias": igate_bias, "fgate_bias": fgate_bias, "memory": memory, "normalizer": normalizer, "stabilizer": stabilizer, "w_output": w_output, "mlp_gain": mlp_gain, "w_up": w_up, "w_down": w_down}


norm_eps = 1e-06

def rms_normed(rows, gain):
    wide_rows = rows.astype(jnp.float32)
    scale = lax.rsqrt(lax.optimization_barrier(jnp.mean(wide_rows * wide_rows, axis=-1, keepdims=True)) + norm_eps)
    return (wide_rows * scale * gain).astype(jnp.bfloat16)

def reference(tokens, mix_gain, w_query, w_key, w_value, w_igate, w_fgate, igate_bias, fgate_bias, memory, normalizer, stabilizer, w_output, mlp_gain, w_up, w_down):
    batch_rows = tokens.shape[0]
    normed = rms_normed(tokens, mix_gain)
    queries = (jnp.dot(normed, w_query, preferred_element_type=jnp.float32) * DQK ** (-0.5)).reshape(batch_rows, NH, DQK)
    key_rows = jnp.dot(normed, w_key, preferred_element_type=jnp.float32).reshape(batch_rows, NH, DQK)
    values = jnp.dot(normed, w_value, preferred_element_type=jnp.float32).reshape(batch_rows, NH, DV)
    input_gate = jnp.dot(normed, w_igate, preferred_element_type=jnp.float32) + igate_bias
    log_forget = jax.nn.log_sigmoid(jnp.dot(normed, w_fgate, preferred_element_type=jnp.float32) + fgate_bias)
    carried = log_forget + stabilizer
    new_stabilizer = jnp.maximum(carried, input_gate)
    keep_weight = jnp.exp(carried - new_stabilizer)
    fresh_weight = jnp.exp(input_gate - new_stabilizer)
    recall = jnp.einsum('bhvd,bhd->bhv', memory, queries, precision=lax.Precision.HIGHEST)
    match_score = lax.optimization_barrier(jnp.sum(queries * key_rows, axis=-1))
    numerator = keep_weight[..., None] * recall + (fresh_weight * match_score)[..., None] * values
    denominator = keep_weight * lax.optimization_barrier(jnp.sum(normalizer * queries, axis=-1)) + fresh_weight * match_score
    floor_value = jnp.maximum(jnp.abs(denominator), jnp.exp(-new_stabilizer))
    cell_out = (numerator / floor_value[..., None]).astype(jnp.bfloat16).reshape(batch_rows, NH * DV)
    new_memory = keep_weight[..., None, None] * memory + fresh_weight[..., None, None] * values[..., :, None] * key_rows[..., None, :]
    new_normalizer = keep_weight[..., None] * normalizer + fresh_weight[..., None] * key_rows
    half_width = NH * DV // N_TP
    summed = tokens.astype(jnp.float32)
    for half_index in range(N_TP):
        half_out = jnp.dot(cell_out[:, half_index * half_width:(half_index + 1) * half_width], w_output[half_index * half_width:(half_index + 1) * half_width], preferred_element_type=jnp.float32).astype(jnp.bfloat16)
        half_out = lax.optimization_barrier(half_out)
        summed = summed + half_out.astype(jnp.float32)
    middle = summed.astype(jnp.bfloat16)
    mixer_in = rms_normed(middle, mlp_gain)
    up_rows = jnp.dot(mixer_in, w_up, preferred_element_type=jnp.float32)
    activation = jnp.square(jax.nn.relu(up_rows)).astype(jnp.bfloat16)
    down_rows = jnp.dot(activation, w_down, preferred_element_type=jnp.float32)
    new_tokens = (middle.astype(jnp.float32) + down_rows).astype(jnp.bfloat16)
    return (new_tokens, new_memory, new_normalizer, new_stabilizer)
```

```python
import functools

import jax
import jax.numpy as jnp
from jax import lax
from jax.experimental import pallas as pl
from jax.experimental.pallas import tpu as pltpu
from jax.sharding import PartitionSpec as P

MESH = pl.DeviceIdType.MESH
F32 = jnp.float32
BF16 = jnp.bfloat16
LANES = 128


norm_eps = 1e-06


def rms_normed(rows, gain):
    wide_rows = rows.astype(jnp.float32)
    scale = lax.rsqrt(jnp.mean(wide_rows * wide_rows, axis=-1, keepdims=True) + norm_eps)
    return (wide_rows * scale * gain).astype(jnp.bfloat16)


def on_device(
    tokens,
    mix_gain,
    w_query,
    w_key,
    w_value,
    w_igate,
    w_fgate,
    igate_bias,
    fgate_bias,
    memory,
    normalizer,
    stabilizer,
    w_output,
    mlp_gain,
    w_up,
    w_down,
):
    DV, DQK = memory.shape[2:]
    kv_count = lax.axis_size("kv")
    tp_count = lax.axis_size("tp")
    kv_index = lax.axis_index("kv")
    tp_index = lax.axis_index("tp")
    own_rows = memory.shape[0]
    head_count = memory.shape[1]
    whole_rows = lax.all_gather(tokens, ("kv", "tp"), axis=1, tiled=True)
    batch_rows = whole_rows.shape[0]
    wide_rows = whole_rows.astype(jnp.float32)
    normed = rms_normed(whole_rows, mix_gain)
    row_span = w_query.shape[0]
    own_cols = lax.dynamic_slice_in_dim(normed, kv_index * row_span, row_span, 1)
    joined = lax.psum_scatter(
        jnp.concatenate(
            [
                jnp.dot(own_cols, w_query, preferred_element_type=jnp.float32),
                jnp.dot(own_cols, w_key, preferred_element_type=jnp.float32),
                jnp.dot(own_cols, w_value, preferred_element_type=jnp.float32),
            ],
            axis=1,
        ),
        "kv",
        scatter_dimension=0,
        tiled=True,
    )
    query_cols = w_query.shape[1]
    queries = joined[:, :query_cols].reshape(own_rows, head_count, DQK) * DQK ** (-0.5)
    key_rows = joined[:, query_cols : 2 * query_cols].reshape(own_rows, head_count, DQK)
    values = joined[:, 2 * query_cols :].reshape(own_rows, head_count, DV)
    own_normed = lax.dynamic_slice_in_dim(normed, kv_index * own_rows, own_rows, 0)
    igate_cols = lax.dynamic_slice_in_dim(w_igate, tp_index * head_count, head_count, 1)
    fgate_cols = lax.dynamic_slice_in_dim(w_fgate, tp_index * head_count, head_count, 1)
    ibias_own = lax.dynamic_slice_in_dim(igate_bias, tp_index * head_count, head_count, 0)
    fbias_own = lax.dynamic_slice_in_dim(fgate_bias, tp_index * head_count, head_count, 0)
    input_gate = jnp.dot(own_normed, igate_cols, preferred_element_type=jnp.float32) + ibias_own
    log_forget = jax.nn.log_sigmoid(
        jnp.dot(own_normed, fgate_cols, preferred_element_type=jnp.float32) + fbias_own
    )
    carried = log_forget + stabilizer
    new_stabilizer = jnp.maximum(carried, input_gate)
    keep_weight = jnp.exp(carried - new_stabilizer)
    fresh_weight = jnp.exp(input_gate - new_stabilizer)
    recall = jnp.einsum("bhvd,bhd->bhv", memory, queries, precision=lax.Precision.HIGHEST)
    match_score = jnp.sum(queries * key_rows, axis=-1)
    numerator = keep_weight[..., None] * recall + (fresh_weight * match_score)[..., None] * values
    denominator = keep_weight * jnp.sum(normalizer * queries, axis=-1) + fresh_weight * match_score
    floor_value = jnp.maximum(jnp.abs(denominator), jnp.exp(-new_stabilizer))
    cell_out = (
        (numerator / floor_value[..., None]).astype(jnp.bfloat16).reshape(own_rows, head_count * DV)
    )
    new_memory = (
        keep_weight[..., None, None] * memory
        + fresh_weight[..., None, None] * values[..., :, None] * key_rows[..., None, :]
    )
    new_normalizer = keep_weight[..., None] * normalizer + fresh_weight[..., None] * key_rows
    partial_value = jnp.dot(
        lax.all_gather(cell_out, "kv", axis=0, tiled=True),
        w_output,
        preferred_element_type=jnp.float32,
    )
    block_cols = partial_value.shape[1]
    pieces = lax.all_gather(
        partial_value.astype(jnp.bfloat16)[:, None, :], ("kv", "tp"), axis=1, tiled=True
    )
    summed = jnp.sum(
        pieces.astype(jnp.float32).reshape(batch_rows, kv_count, tp_count, block_cols), axis=2
    )
    middle = (wide_rows + summed.reshape(batch_rows, kv_count * block_cols)).astype(jnp.bfloat16)
    mixer_in = rms_normed(middle, mlp_gain)
    up_rows = jnp.dot(mixer_in, w_up, preferred_element_type=jnp.float32)
    activation = jnp.square(jax.nn.relu(up_rows)).astype(jnp.bfloat16)
    thin_cols = tokens.shape[1]
    down_cols = lax.psum_scatter(
        lax.dot_general(
            w_down, activation, (((0,), (1,)), ((), ())), preferred_element_type=jnp.float32
        ),
        ("kv", "tp"),
        scatter_dimension=0,
        tiled=True,
    )
    middle_own = lax.dynamic_slice_in_dim(
        middle, (kv_index * tp_count + tp_index) * thin_cols, thin_cols, 1
    )
    new_tokens = (middle_own.astype(jnp.float32) + down_cols.T).astype(jnp.bfloat16)
    return (new_tokens, new_memory, new_normalizer, new_stabilizer)


def fused_cell(
    n_kv,
    n_tp,
    tok_h, mixg_h, wq_h, wk_h, wv_h, wig_h, wfg_h, ib_h, fb_h,
    mem_h, nrm_h, stb_h, wo_h, mlpg_h, wup_h, wdn_h,
    otok, omem_h, onrm, ostb,
    tok, tokall, mixg, wq, wk, wv, wig, wfg, ib, fb,
    mem, membf, newmem, nrm, stb, wo, mlpg, wup, wdn,
    snd, rcv, cell_own, cell_all, y_own, y_all, mid, acc, act, stage, land,
    small_sem, w_sem, up_sem, out_sem,
    tok_s, tok_r, rs_s, rs_r, cell_s, cell_r, y_s, y_r, dn_s, dn_r,
):
    dp = lax.axis_index("dp")
    kv = lax.axis_index("kv")
    tp = lax.axis_index("tp")
    n_all = n_kv * n_tp
    g = kv * n_tp + tp
    batch, thin = tok.shape
    span = wq.shape[0]
    heads, dv, dqk = mem.shape
    width = tokall.shape[0] * thin
    halves = dv // LANES

    def peer_of(offset):
        other = (g + offset) % n_all
        return other, (dp, other // n_tp, other % n_tp)

    barrier = pltpu.get_barrier_semaphore()
    for o in range(1, n_all):
        pl.semaphore_signal(barrier, inc=1, device_id=peer_of(o)[1], device_id_type=MESH)

    own_span = pl.ds(pl.multiple_of(kv * span, span), span)
    smalls = [
        (tok_h, tok), (mixg_h, mixg), (wig_h.at[own_span], wig), (wfg_h.at[own_span], wfg),
        (ib_h, ib), (fb_h, fb), (nrm_h.at[0], nrm), (stb_h, stb), (mlpg_h, mlpg),
    ]
    small = [pltpu.make_async_copy(a, b, small_sem.at[i]) for i, (a, b) in enumerate(smalls)]
    bigs = [(wq_h, wq), (wk_h, wk), (wv_h, wv), (mem_h.at[0], mem), (wo_h, wo), (wdn_h, wdn)]
    big = [pltpu.make_async_copy(a, b, w_sem.at[i]) for i, (a, b) in enumerate(bigs)]
    for c in small:
        c.start()
    for c in big[:5]:
        c.start()

    def up_rows(i):
        off = i + (i // 2) * (5 - 2 * i) if n_kv == 4 else i
        j = (kv + off) % n_kv
        return j, pl.ds(pl.multiple_of(j * span, span), span)

    def up_copy(i):
        j, rows = up_rows(i)
        return pltpu.make_async_copy(wup_h.at[rows], wup.at[rows], up_sem.at[j])

    small[0].wait()
    pl.semaphore_wait(barrier, n_all - 1)

    def tok_copy(o):
        return pltpu.make_async_remote_copy(
            src_ref=tok, dst_ref=tokall.at[g], send_sem=tok_s.at[o], recv_sem=tok_r.at[g],
            device_id=peer_of(o)[1], device_id_type=MESH)

    def tok_wait(src):
        pltpu.make_async_remote_copy(
            src_ref=tok, dst_ref=tokall.at[src], send_sem=tok_s.at[0], recv_sem=tok_r.at[src],
            device_id=peer_of(1)[1], device_id_type=MESH).wait_recv()

    mate = [(kv * n_tp + (tp + t) % n_tp) for t in range(1, n_tp)]
    for src in mate:
        pltpu.make_async_remote_copy(
            src_ref=tok, dst_ref=tokall.at[g], send_sem=tok_s.at[src], recv_sem=tok_r.at[g],
            device_id=(dp, kv, src % n_tp), device_id_type=MESH).start()
    tokall[g] = tok[...]

    def far_tok(o, t):
        to = (kv + o) % n_kv
        other = to * n_tp + (tp + t) % n_tp
        return other, pltpu.make_async_remote_copy(
            src_ref=tok, dst_ref=tokall.at[g], send_sem=tok_s.at[other], recv_sem=tok_r.at[g],
            device_id=(dp, to, (tp + t) % n_tp), device_id_type=MESH)

    for o in range(1, n_kv):
        for t in range(n_tp):
            far_tok(o, t)[1].start()

    snd[:, heads : 2 * heads, :] = jnp.zeros((n_kv, heads, LANES), F32)
    for src in mate:
        tok_wait(src)
    for c in small[1:]:
        c.wait()

    def chunk(t):
        return tokall[kv * n_tp + t].astype(F32)

    raw = jnp.concatenate([chunk(t) for t in range(n_tp)], axis=1)
    x = (raw * mixg[:, own_span]).astype(BF16)
    squares = jnp.sum(raw * raw, axis=1, keepdims=True)
    snd[:, heads + 2, :] = jnp.broadcast_to(squares, (n_kv, LANES))
    gate_count = wig.shape[1]
    snd[:, heads, :gate_count] = jnp.dot(x, wig[...], preferred_element_type=F32)
    snd[:, heads + 1, :gate_count] = jnp.dot(x, wfg[...], preferred_element_type=F32)

    pieces = [(0, 2 * heads), (2 * heads, heads), (3 * heads, halves * heads)]

    def rs_copy(o, p):
        first, size = pieces[p]
        to = (kv + o) % n_kv
        return pltpu.make_async_remote_copy(
            src_ref=snd.at[to, pl.ds(first, size)],
            dst_ref=rcv.at[o, pl.ds(first, size)],
            send_sem=rs_s.at[o, p], recv_sem=rs_r.at[o, p],
            device_id=(dp, to, tp), device_id_type=MESH)

    far_first = sorted(range(1, n_kv), key=lambda o: -min(o, n_kv - o))
    big[0].wait()
    q_part = jnp.dot(x, wq[...], preferred_element_type=F32)
    for h in range(heads):
        snd[:, h, :] = q_part[:, h * dqk : (h + 1) * dqk]
    for o in far_first:
        rs_copy(o, 0).start()
    big[1].wait()
    up_copy(0).start()
    up_copy(1).start()
    k_part = jnp.dot(x, wk[...], preferred_element_type=F32)
    for h in range(heads):
        snd[:, 2 * heads + h, :] = k_part[:, h * dqk : (h + 1) * dqk]
    for o in far_first:
        rs_copy(o, 1).start()
    big[2].wait()
    for i in range(2, n_kv):
        up_copy(i).start()
    v_part = jnp.dot(x, wv[...], preferred_element_type=F32)
    for h in range(heads):
        for s in range(halves):
            at = h * dv + s * LANES
            snd[:, (3 + s) * heads + h, :] = v_part[:, at : at + LANES]
    for o in far_first:
        rs_copy(o, 2).start()
    big[5].start()
    big[3].wait()
    membf[...] = mem[...].astype(BF16).reshape(heads * dv, dqk)

    lane = lax.broadcasted_iota(jnp.int32, (heads, LANES), 1)
    sub = lax.broadcasted_iota(jnp.int32, (heads, LANES), 0)
    own_head = lane == sub + tp * heads

    def column(row):
        wide = jnp.pad(row, ((0, 0), (0, LANES - row.shape[1]))) if row.shape[1] < LANES else row
        return jnp.sum(jnp.where(own_head, jnp.broadcast_to(wide, own_head.shape), 0.0), axis=1, keepdims=True)

    def joined(p):
        first, size = pieces[p]
        total = snd[kv, first : first + size, :]
        for o in range(1, n_kv):
            rs_copy(o, p).wait_recv()
            total = total + rcv[o, first : first + size, :]
        return total

    part = joined(0)
    scale = lax.rsqrt(part[heads + 2 : heads + 3] * (1.0 / width) + norm_eps)
    q = part[:heads] * scale * dqk**-0.5
    gate_i = column(part[heads : heads + 1] * scale) + column(ib[...])
    gate_f = column(part[heads + 1 : heads + 2] * scale) + column(fb[...])
    log_forget = jnp.minimum(gate_f, 0.0) - jnp.log1p(jnp.exp(-jnp.abs(gate_f)))
    stab_wide = jnp.broadcast_to(stb[...], (heads, heads))
    eye = (lax.broadcasted_iota(jnp.int32, (heads, heads), 0)
           == lax.broadcasted_iota(jnp.int32, (heads, heads), 1))
    stab = jnp.sum(jnp.where(eye, stab_wide, 0.0), axis=1, keepdims=True)
    carried = log_forget + stab
    new_stab = jnp.maximum(carried, gate_i)
    keep = jnp.exp(carried - new_stab)
    fresh = jnp.exp(gate_i - new_stab)
    ostb[...] = jnp.sum(jnp.where(eye, jnp.broadcast_to(new_stab, (heads, heads)), 0.0), axis=0, keepdims=True)
    norm_dot = jnp.sum(nrm[...] * q, axis=1, keepdims=True)
    q_hi = q.astype(BF16)
    q_lo = (q - q_hi.astype(F32)).astype(BF16)
    wide_recall = lax.dot_general(
        jnp.concatenate([q_hi, q_lo], axis=0), membf[...], (((1,), (1,)), ((), ())),
        preferred_element_type=F32)
    wide_recall = wide_recall[:heads] + wide_recall[heads:]
    row_id = lax.broadcasted_iota(jnp.int32, (heads, dv), 0)
    recall = jnp.zeros((heads, dv), F32)
    for h in range(heads):
        recall = jnp.where(row_id == h, wide_recall[:, h * dv : (h + 1) * dv], recall)
    k = joined(1) * scale
    match = jnp.sum(q * k, axis=1, keepdims=True)
    denominator = keep * norm_dot + fresh * match
    floor_value = jnp.maximum(jnp.abs(denominator), jnp.exp(-new_stab))
    v_rows = joined(2)
    v = jnp.concatenate([v_rows[s * heads : (s + 1) * heads] * scale for s in range(halves)], axis=1)
    cell = (keep * recall + (fresh * match) * v) / floor_value
    cell_own[...] = cell

    def cell_copy(o):
        to = (kv + o) % n_kv
        return pltpu.make_async_remote_copy(
            src_ref=cell_own, dst_ref=cell_all.at[kv], send_sem=cell_s.at[o], recv_sem=cell_r.at[o],
            device_id=(dp, to, tp), device_id_type=MESH)

    for o in far_first:
        cell_copy(o).start()
    cell_all[kv] = cell
    onrm[0] = keep * nrm[...] + fresh * k
    fresh_v = fresh * v
    fresh_vt = fresh_v.T
    for h in range(heads):
        newmem[h] = keep[h : h + 1] * mem[h] + fresh_vt[:, h : h + 1] * k[h : h + 1]
    out_mem = pltpu.make_async_copy(newmem, omem_h.at[0], out_sem.at[0])
    out_mem.start()
    big[4].wait()
    for o in range(1, n_kv):
        src = (kv + n_kv - o) % n_kv
        pltpu.make_async_remote_copy(
            src_ref=cell_own, dst_ref=cell_all.at[src], send_sem=cell_s.at[o], recv_sem=cell_r.at[o],
            device_id=(dp, src, tp), device_id_type=MESH).wait_recv()
    rows = jnp.concatenate([cell_all[:, h, :] for h in range(heads)], axis=1).astype(BF16)
    y = jnp.dot(rows, wo[...], preferred_element_type=F32).astype(BF16)
    y_own[...] = y

    def y_copy(o, t):
        to = (kv + o) % n_kv
        to_tp = (tp + t) % n_tp
        return pltpu.make_async_remote_copy(
            src_ref=y_own, dst_ref=y_all.at[g], send_sem=y_s.at[to * n_tp + to_tp], recv_sem=y_r.at[g],
            device_id=(dp, to, to_tp), device_id_type=MESH)

    for o in far_first + [0]:
        for t in range(n_tp):
            if o or t:
                y_copy(o, t).start()
    y_all[g] = y
    for o in range(1, n_kv):
        for t in range(n_tp):
            tok_wait(((kv + o) % n_kv) * n_tp + (tp + t) % n_tp)

    def y_wait(src):
        pltpu.make_async_remote_copy(
            src_ref=y_own, dst_ref=y_all.at[src], send_sem=y_s.at[0], recv_sem=y_r.at[src],
            device_id=peer_of(1)[1], device_id_type=MESH).wait_recv()

    def up_step(i, square_sum):
        j, span_rows = up_rows(i)
        up_copy(i).wait()
        for t in range(1, n_tp):
            y_wait(j * n_tp + (tp + t) % n_tp)

        @pl.when(i > 0)
        def _():
            y_wait(j * n_tp + tp)

        base = jnp.concatenate([tokall[j * n_tp + t].astype(F32) for t in range(n_tp)], axis=1)
        for t in range(n_tp):
            base = base + y_all[j * n_tp + t].astype(F32)
        m = base.astype(BF16).astype(F32)
        mid[j] = m
        mixed = (m * mlpg[:, span_rows]).astype(BF16)
        part = jnp.dot(mixed, wup[span_rows, :], preferred_element_type=F32)

        @pl.when(i == 0)
        def _():
            acc[...] = part

        @pl.when(i > 0)
        def _():
            acc[...] += part

        return square_sum + jnp.sum(m * m, axis=1, keepdims=True)

    square_sum = lax.fori_loop(0, n_kv, up_step, jnp.zeros((batch, 1), F32))
    scale2 = lax.rsqrt(square_sum * (1.0 / width) + norm_eps)
    up = jnp.maximum(acc[...] * scale2, 0.0)
    act[...] = (up * up).astype(BF16)
    big[5].wait()

    def dn_copy(o):
        return pltpu.make_async_remote_copy(
            src_ref=stage.at[o], dst_ref=land.at[o], send_sem=dn_s.at[o], recv_sem=dn_r.at[o],
            device_id=peer_of(o)[1], device_id_type=MESH)

    def down_step(i, carry):
        o = 1 + (i + n_all // 2 - 1) % (n_all - 1) + (i // (n_all - 1)) * (n_all - 1 - (n_all // 2 - 1))
        o = o % n_all
        other, _ = peer_of(o)
        cols = pl.ds(pl.multiple_of(other * thin, thin), thin)
        stage[o] = jnp.dot(act[...], wdn[:, cols], preferred_element_type=F32)

        @pl.when(i < n_all - 1)
        def _():
            dn_copy(o).start()

        return carry

    lax.fori_loop(0, n_all, down_step, 0)
    total = mid[kv, :, pl.ds(pl.multiple_of(tp * thin, thin), thin)] + stage[0]
    for o in range(1, n_all):
        dn_copy(o).wait_recv()
        total = total + land[o]
    otok[...] = total.astype(BF16)

    for src in mate:
        pltpu.make_async_remote_copy(
            src_ref=tok, dst_ref=tokall.at[g], send_sem=tok_s.at[src], recv_sem=tok_r.at[g],
            device_id=(dp, kv, src % n_tp), device_id_type=MESH).wait_send()
    for o in range(n_kv):
        for t in range(n_tp):
            if o:
                far_tok(o, t)[1].wait_send()
            if o or t:
                y_copy(o, t).wait_send()
        if o:
            for p in range(len(pieces)):
                rs_copy(o, p).wait_send()
            cell_copy(o).wait_send()
    for o in range(1, n_all):
        dn_copy(o).wait_send()
    out_mem.wait()


def fits_fused(tokens, w_query, w_value, memory, w_output, w_up, w_down, n_kv, n_tp):
    own_rows, heads, dv, dqk = memory.shape
    batch, thin = tokens.shape
    span = w_query.shape[0]
    held = 2 * (2 * w_query.size + w_value.size + w_output.size + w_up.size + w_down.size)
    held += 10 * memory.size
    return (
        own_rows == 1 and batch == n_kv and heads == 8 and dqk == LANES and dv % LANES == 0
        and thin % LANES == 0 and span == n_tp * thin and n_kv >= 2 and n_tp >= 2
        and w_output.shape[1] == span and held < 52 * 2**20
    )


def fused_on_device(
    tokens, mix_gain, w_query, w_key, w_value, w_igate, w_fgate, igate_bias, fgate_bias,
    memory, normalizer, stabilizer, w_output, mlp_gain, w_up, w_down,
):
    n_kv = lax.axis_size("kv")
    n_tp = lax.axis_size("tp")
    n_all = n_kv * n_tp
    batch, thin = tokens.shape
    _, heads, dv, dqk = memory.shape
    span = w_query.shape[0]
    width = n_all * thin
    halves = dv // LANES
    groups = (3 + halves) * heads
    hidden = w_up.shape[1]
    any_spec = pl.BlockSpec(memory_space=pl.ANY)
    vmem_spec = pl.BlockSpec(memory_space=pltpu.VMEM)
    vm = pltpu.VMEM
    dma = pltpu.SemaphoreType.DMA
    scratch = [
        vm((batch, thin), BF16),
        vm((n_all, batch, thin), BF16),
        vm((1, width), F32),
        vm(w_query.shape, BF16),
        vm(w_key.shape, BF16),
        vm(w_value.shape, BF16),
        vm((span, w_igate.shape[1]), BF16),
        vm((span, w_fgate.shape[1]), BF16),
        vm((1, igate_bias.shape[0]), F32),
        vm((1, fgate_bias.shape[0]), F32),
        vm((heads, dv, dqk), F32),
        vm((heads * dv, dqk), BF16),
        vm((heads, dv, dqk), F32),
        vm((heads, dqk), F32),
        vm((1, heads), F32),
        vm(w_output.shape, BF16),
        vm((1, width), F32),
        vm(w_up.shape, BF16),
        vm(w_down.shape, BF16),
        vm((n_kv, groups, LANES), F32),
        vm((n_kv, groups, LANES), F32),
        vm((heads, dv), F32),
        vm((n_kv, heads, dv), F32),
        vm((batch, span), BF16),
        vm((n_all, batch, span), BF16),
        vm((n_kv, batch, span), F32),
        vm((batch, hidden), F32),
        vm((batch, hidden), BF16),
        vm((n_all, batch, thin), F32),
        vm((n_all, batch, thin), F32),
        dma((9,)), dma((6,)), dma((n_kv,)), dma((1,)),
        dma((n_all,)), dma((n_all,)),
        dma((n_kv, 3)), dma((n_kv, 3)),
        dma((n_kv,)), dma((n_kv,)),
        dma((n_all,)), dma((n_all,)),
        dma((n_all,)), dma((n_all,)),
    ]
    return pl.pallas_call(
        functools.partial(fused_cell, n_kv, n_tp),
        out_shape=(
            jax.ShapeDtypeStruct(tokens.shape, BF16),
            jax.ShapeDtypeStruct(memory.shape, F32),
            jax.ShapeDtypeStruct(normalizer.shape, F32),
            jax.ShapeDtypeStruct(stabilizer.shape, F32),
        ),
        in_specs=[any_spec] * 16,
        out_specs=(vmem_spec, any_spec, vmem_spec, vmem_spec),
        scratch_shapes=scratch,
        compiler_params=pltpu.CompilerParams(
            collective_id=0, has_side_effects=True, vmem_limit_bytes=60 * 2**20
        ),
        name="fused_cell",
    )(
        tokens, mix_gain.reshape(1, -1), w_query, w_key, w_value, w_igate, w_fgate,
        igate_bias.reshape(1, -1), fgate_bias.reshape(1, -1), memory, normalizer, stabilizer,
        w_output, mlp_gain.reshape(1, -1), w_up, w_down,
    )


def routed(*arrays):
    tokens, w_query, w_value, memory = arrays[0], arrays[2], arrays[4], arrays[9]
    w_output, w_up, w_down = arrays[12], arrays[14], arrays[15]
    n_kv, n_tp = lax.axis_size("kv"), lax.axis_size("tp")
    if fits_fused(tokens, w_query, w_value, memory, w_output, w_up, w_down, n_kv, n_tp):
        return fused_on_device(*arrays)
    return on_device(*arrays)


def solution(mesh):
    in_specs = (
        P("dp", ("kv", "tp")),
        P(),
        P("kv", "tp"),
        P("kv", "tp"),
        P("kv", "tp"),
        P(),
        P(),
        P(),
        P(),
        P(("dp", "kv"), "tp", None, None),
        P(("dp", "kv"), "tp", None),
        P(("dp", "kv"), "tp"),
        P("tp", "kv"),
        P(),
        P(None, ("kv", "tp")),
        P(("kv", "tp"), None),
    )
    out_specs = (
        P("dp", ("kv", "tp")),
        P(("dp", "kv"), "tp", None, None),
        P(("dp", "kv"), "tp", None),
        P(("dp", "kv"), "tp"),
    )
    return jax.shard_map(
        routed, mesh=mesh, in_specs=in_specs, out_specs=out_specs, check_vma=False
    )
```

```python
import functools

import jax
import jax.numpy as jnp
from jax import lax
from jax.experimental import pallas as pl
from jax.experimental.pallas import tpu as pltpu
from jax.sharding import PartitionSpec as P

MESH = pl.DeviceIdType.MESH
F32 = jnp.float32
BF16 = jnp.bfloat16
LANES = 128


norm_eps = 1e-06


def rms_normed(rows, gain):
    wide_rows = rows.astype(jnp.float32)
    scale = lax.rsqrt(jnp.mean(wide_rows * wide_rows, axis=-1, keepdims=True) + norm_eps)
    return (wide_rows * scale * gain).astype(jnp.bfloat16)


def on_device(
    tokens,
    mix_gain,
    w_query,
    w_key,
    w_value,
    w_igate,
    w_fgate,
    igate_bias,
    fgate_bias,
    memory,
    normalizer,
    stabilizer,
    w_output,
    mlp_gain,
    w_up,
    w_down,
):
    DV, DQK = memory.shape[2:]
    kv_count = lax.axis_size("kv")
    tp_count = lax.axis_size("tp")
    kv_index = lax.axis_index("kv")
    tp_index = lax.axis_index("tp")
    own_rows = memory.shape[0]
    head_count = memory.shape[1]
    whole_rows = lax.all_gather(tokens, ("kv", "tp"), axis=1, tiled=True)
    batch_rows = whole_rows.shape[0]
    wide_rows = whole_rows.astype(jnp.float32)
    normed = rms_normed(whole_rows, mix_gain)
    row_span = w_query.shape[0]
    own_cols = lax.dynamic_slice_in_dim(normed, kv_index * row_span, row_span, 1)
    joined = lax.psum_scatter(
        jnp.concatenate(
            [
                jnp.dot(own_cols, w_query, preferred_element_type=jnp.float32),
                jnp.dot(own_cols, w_key, preferred_element_type=jnp.float32),
                jnp.dot(own_cols, w_value, preferred_element_type=jnp.float32),
            ],
            axis=1,
        ),
        "kv",
        scatter_dimension=0,
        tiled=True,
    )
    query_cols = w_query.shape[1]
    queries = joined[:, :query_cols].reshape(own_rows, head_count, DQK) * DQK ** (-0.5)
    key_rows = joined[:, query_cols : 2 * query_cols].reshape(own_rows, head_count, DQK)
    values = joined[:, 2 * query_cols :].reshape(own_rows, head_count, DV)
    own_normed = lax.dynamic_slice_in_dim(normed, kv_index * own_rows, own_rows, 0)
    igate_cols = lax.dynamic_slice_in_dim(w_igate, tp_index * head_count, head_count, 1)
    fgate_cols = lax.dynamic_slice_in_dim(w_fgate, tp_index * head_count, head_count, 1)
    ibias_own = lax.dynamic_slice_in_dim(igate_bias, tp_index * head_count, head_count, 0)
    fbias_own = lax.dynamic_slice_in_dim(fgate_bias, tp_index * head_count, head_count, 0)
    input_gate = jnp.dot(own_normed, igate_cols, preferred_element_type=jnp.float32) + ibias_own
    log_forget = jax.nn.log_sigmoid(
        jnp.dot(own_normed, fgate_cols, preferred_element_type=jnp.float32) + fbias_own
    )
    carried = log_forget + stabilizer
    new_stabilizer = jnp.maximum(carried, input_gate)
    keep_weight = jnp.exp(carried - new_stabilizer)
    fresh_weight = jnp.exp(input_gate - new_stabilizer)
    recall = jnp.einsum("bhvd,bhd->bhv", memory, queries, precision=lax.Precision.HIGHEST)
    match_score = jnp.sum(queries * key_rows, axis=-1)
    numerator = keep_weight[..., None] * recall + (fresh_weight * match_score)[..., None] * values
    denominator = keep_weight * jnp.sum(normalizer * queries, axis=-1) + fresh_weight * match_score
    floor_value = jnp.maximum(jnp.abs(denominator), jnp.exp(-new_stabilizer))
    cell_out = (
        (numerator / floor_value[..., None]).astype(jnp.bfloat16).reshape(own_rows, head_count * DV)
    )
    new_memory = (
        keep_weight[..., None, None] * memory
        + fresh_weight[..., None, None] * values[..., :, None] * key_rows[..., None, :]
    )
    new_normalizer = keep_weight[..., None] * normalizer + fresh_weight[..., None] * key_rows
    partial_value = jnp.dot(
        lax.all_gather(cell_out, "kv", axis=0, tiled=True),
        w_output,
        preferred_element_type=jnp.float32,
    )
    block_cols = partial_value.shape[1]
    pieces = lax.all_gather(
        partial_value.astype(jnp.bfloat16)[:, None, :], ("kv", "tp"), axis=1, tiled=True
    )
    summed = jnp.sum(
        pieces.astype(jnp.float32).reshape(batch_rows, kv_count, tp_count, block_cols), axis=2
    )
    middle = (wide_rows + summed.reshape(batch_rows, kv_count * block_cols)).astype(jnp.bfloat16)
    mixer_in = rms_normed(middle, mlp_gain)
    up_rows = jnp.dot(mixer_in, w_up, preferred_element_type=jnp.float32)
    activation = jnp.square(jax.nn.relu(up_rows)).astype(jnp.bfloat16)
    thin_cols = tokens.shape[1]
    down_cols = lax.psum_scatter(
        lax.dot_general(
            w_down, activation, (((0,), (1,)), ((), ())), preferred_element_type=jnp.float32
        ),
        ("kv", "tp"),
        scatter_dimension=0,
        tiled=True,
    )
    middle_own = lax.dynamic_slice_in_dim(
        middle, (kv_index * tp_count + tp_index) * thin_cols, thin_cols, 1
    )
    new_tokens = (middle_own.astype(jnp.float32) + down_cols.T).astype(jnp.bfloat16)
    return (new_tokens, new_memory, new_normalizer, new_stabilizer)


def fused_cell(
    n_kv,
    n_tp,
    tok_h, mixg_h, wq_h, wk_h, wv_h, wig_h, wfg_h, ib_h, fb_h,
    mem_h, nrm_h, stb_h, wo_h, mlpg_h, wup_h, wdn_h,
    otok, newmem, onrm, ostb,
    tok, tokall, mixg, wq, wk, wv, wig, wfg, ib, fb,
    mem, membf, nrm, stb, wo, mlpg, wup, wdn,
    snd, rcv, cell_own, cell_all, y_own, y_all, mid, acc, act, stage, land,
    small_sem, w_sem, up_sem,
    tok_s, tok_r, rs_s, rs_r, cell_s, cell_r, y_s, y_r, dn_s, dn_r,
):
    dp = lax.axis_index("dp")
    kv = lax.axis_index("kv")
    tp = lax.axis_index("tp")
    n_all = n_kv * n_tp
    g = kv * n_tp + tp
    batch, thin = tok.shape
    span = wq.shape[0]
    heads, dv, dqk = mem.shape
    width = tokall.shape[0] * thin
    halves = dv // LANES

    def peer_of(offset):
        other = (g + offset) % n_all
        return other, (dp, other // n_tp, other % n_tp)

    barrier = pltpu.get_barrier_semaphore()
    for o in range(1, n_all):
        pl.semaphore_signal(barrier, inc=1, device_id=peer_of(o)[1], device_id_type=MESH)

    own_span = pl.ds(pl.multiple_of(kv * span, span), span)
    smalls = [
        (tok_h, tok), (mixg_h, mixg), (wig_h.at[:, own_span], wig), (wfg_h.at[:, own_span], wfg),
        (ib_h, ib), (fb_h, fb), (nrm_h.at[0], nrm), (stb_h, stb), (mlpg_h, mlpg),
    ]
    small = [pltpu.make_async_copy(a, b, small_sem.at[i]) for i, (a, b) in enumerate(smalls)]
    bigs = [(wq_h, wq), (wk_h, wk), (wv_h, wv), (mem_h.at[0], mem), (wo_h, wo), (wdn_h, wdn)]
    big = [pltpu.make_async_copy(a, b, w_sem.at[i]) for i, (a, b) in enumerate(bigs)]
    for c in small:
        c.start()
    for c in big[:5]:
        c.start()

    def up_rows(i):
        off = i + (i // 2) * (5 - 2 * i) if n_kv == 4 else i
        j = (kv + off) % n_kv
        return j, pl.ds(pl.multiple_of(j * span, span), span)

    def up_copy(i):
        j, rows = up_rows(i)
        return pltpu.make_async_copy(wup_h.at[rows], wup.at[rows], up_sem.at[j])

    small[0].wait()
    pl.semaphore_wait(barrier, n_all - 1)

    def tok_copy(o):
        return pltpu.make_async_remote_copy(
            src_ref=tok, dst_ref=tokall.at[g], send_sem=tok_s.at[o], recv_sem=tok_r.at[g],
            device_id=peer_of(o)[1], device_id_type=MESH)

    def tok_wait(src):
        pltpu.make_async_remote_copy(
            src_ref=tok, dst_ref=tokall.at[src], send_sem=tok_s.at[0], recv_sem=tok_r.at[src],
            device_id=peer_of(1)[1], device_id_type=MESH).wait_recv()

    mate = [(kv * n_tp + (tp + t) % n_tp) for t in range(1, n_tp)]
    for src in mate:
        pltpu.make_async_remote_copy(
            src_ref=tok, dst_ref=tokall.at[g], send_sem=tok_s.at[src], recv_sem=tok_r.at[g],
            device_id=(dp, kv, src % n_tp), device_id_type=MESH).start()
    tokall[g] = tok[...]

    def far_tok(o, t):
        to = (kv + o) % n_kv
        other = to * n_tp + (tp + t) % n_tp
        return other, pltpu.make_async_remote_copy(
            src_ref=tok, dst_ref=tokall.at[g], send_sem=tok_s.at[other], recv_sem=tok_r.at[g],
            device_id=(dp, to, (tp + t) % n_tp), device_id_type=MESH)

    for o in range(1, n_kv):
        for t in range(n_tp):
            far_tok(o, t)[1].start()

    snd[:, heads : 2 * heads, :] = jnp.zeros((n_kv, heads, LANES), F32)
    for src in mate:
        tok_wait(src)
    for c in small[1:]:
        c.wait()

    def chunk(t):
        return tokall[kv * n_tp + t].astype(F32)

    raw = jnp.concatenate([chunk(t) for t in range(n_tp)], axis=1)
    x = (raw * mixg[:, own_span]).astype(BF16)
    squares = jnp.sum(raw * raw, axis=1, keepdims=True)
    snd[:, heads + 2, :] = jnp.broadcast_to(squares, (n_kv, LANES))
    gate_count = wig.shape[0]
    last = (((1,), (1,)), ((), ()))
    snd[:, heads, :gate_count] = lax.dot_general(x, wig[...], last, preferred_element_type=F32)
    snd[:, heads + 1, :gate_count] = lax.dot_general(x, wfg[...], last, preferred_element_type=F32)

    pieces = [(0, 2 * heads), (2 * heads, heads), (3 * heads, halves * heads)]

    def rs_copy(o, p):
        first, size = pieces[p]
        to = (kv + o) % n_kv
        return pltpu.make_async_remote_copy(
            src_ref=snd.at[to, pl.ds(first, size)],
            dst_ref=rcv.at[o, pl.ds(first, size)],
            send_sem=rs_s.at[o, p], recv_sem=rs_r.at[o, p],
            device_id=(dp, to, tp), device_id_type=MESH)

    far_first = sorted(range(1, n_kv), key=lambda o: -min(o, n_kv - o))
    big[0].wait()
    q_part = jnp.dot(x, wq[...], preferred_element_type=F32)
    for h in range(heads):
        snd[:, h, :] = q_part[:, h * dqk : (h + 1) * dqk]
    for o in far_first:
        rs_copy(o, 0).start()
    big[1].wait()
    up_copy(0).start()
    up_copy(1).start()
    k_part = jnp.dot(x, wk[...], preferred_element_type=F32)
    for h in range(heads):
        snd[:, 2 * heads + h, :] = k_part[:, h * dqk : (h + 1) * dqk]
    for o in far_first:
        rs_copy(o, 1).start()
    big[2].wait()
    for i in range(2, n_kv):
        up_copy(i).start()
    v_part = jnp.dot(x, wv[...], preferred_element_type=F32)
    for h in range(heads):
        for s in range(halves):
            at = h * dv + s * LANES
            snd[:, (3 + s) * heads + h, :] = v_part[:, at : at + LANES]
    for o in far_first:
        rs_copy(o, 2).start()
    big[5].start()
    big[3].wait()
    membf[...] = mem[...].astype(BF16).reshape(heads * dv, dqk)

    lane = lax.broadcasted_iota(jnp.int32, (heads, LANES), 1)
    sub = lax.broadcasted_iota(jnp.int32, (heads, LANES), 0)
    own_head = lane == sub + tp * heads

    def column(row):
        wide = jnp.pad(row, ((0, 0), (0, LANES - row.shape[1]))) if row.shape[1] < LANES else row
        return jnp.sum(jnp.where(own_head, jnp.broadcast_to(wide, own_head.shape), 0.0), axis=1, keepdims=True)

    def joined(p):
        first, size = pieces[p]
        total = snd[kv, first : first + size, :]
        for o in range(1, n_kv):
            rs_copy(o, p).wait_recv()
            total = total + rcv[o, first : first + size, :]
        return total

    part = joined(0)
    scale = lax.rsqrt(part[heads + 2 : heads + 3] * (1.0 / width) + norm_eps)
    q = part[:heads] * scale * dqk**-0.5
    gate_i = column(part[heads : heads + 1] * scale) + column(ib[...])
    gate_f = column(part[heads + 1 : heads + 2] * scale) + column(fb[...])
    log_forget = jnp.minimum(gate_f, 0.0) - jnp.log1p(jnp.exp(-jnp.abs(gate_f)))
    stab_wide = jnp.broadcast_to(stb[...], (heads, heads))
    eye = (lax.broadcasted_iota(jnp.int32, (heads, heads), 0)
           == lax.broadcasted_iota(jnp.int32, (heads, heads), 1))
    stab = jnp.sum(jnp.where(eye, stab_wide, 0.0), axis=1, keepdims=True)
    carried = log_forget + stab
    new_stab = jnp.maximum(carried, gate_i)
    keep = jnp.exp(carried - new_stab)
    fresh = jnp.exp(gate_i - new_stab)
    ostb[...] = jnp.sum(jnp.where(eye, jnp.broadcast_to(new_stab, (heads, heads)), 0.0), axis=0, keepdims=True)
    norm_dot = jnp.sum(nrm[...] * q, axis=1, keepdims=True)
    q_hi = q.astype(BF16)
    q_lo = (q - q_hi.astype(F32)).astype(BF16)
    wide_recall = lax.dot_general(
        jnp.concatenate([q_hi, q_lo], axis=0), membf[...], (((1,), (1,)), ((), ())),
        preferred_element_type=F32)
    wide_recall = wide_recall[:heads] + wide_recall[heads:]
    row_id = lax.broadcasted_iota(jnp.int32, (heads, dv), 0)
    recall = jnp.zeros((heads, dv), F32)
    for h in range(heads):
        recall = jnp.where(row_id == h, wide_recall[:, h * dv : (h + 1) * dv], recall)
    k = joined(1) * scale
    match = jnp.sum(q * k, axis=1, keepdims=True)
    denominator = keep * norm_dot + fresh * match
    floor_value = jnp.maximum(jnp.abs(denominator), jnp.exp(-new_stab))
    v_rows = joined(2)
    v = jnp.concatenate([v_rows[s * heads : (s + 1) * heads] * scale for s in range(halves)], axis=1)
    cell = (keep * recall + (fresh * match) * v) / floor_value
    cell_own[...] = cell

    def cell_copy(o):
        to = (kv + o) % n_kv
        return pltpu.make_async_remote_copy(
            src_ref=cell_own, dst_ref=cell_all.at[kv], send_sem=cell_s.at[o], recv_sem=cell_r.at[o],
            device_id=(dp, to, tp), device_id_type=MESH)

    for o in far_first:
        cell_copy(o).start()
    cell_all[kv] = cell
    onrm[0] = keep * nrm[...] + fresh * k
    fresh_v = fresh * v
    fresh_vt = fresh_v.T
    for h in range(heads):
        newmem[0, h] = keep[h : h + 1] * mem[h] + fresh_vt[:, h : h + 1] * k[h : h + 1]
    big[4].wait()
    for o in range(1, n_kv):
        src = (kv + n_kv - o) % n_kv
        pltpu.make_async_remote_copy(
            src_ref=cell_own, dst_ref=cell_all.at[src], send_sem=cell_s.at[o], recv_sem=cell_r.at[o],
            device_id=(dp, src, tp), device_id_type=MESH).wait_recv()
    rows = jnp.concatenate([cell_all[:, h, :] for h in range(heads)], axis=1).astype(BF16)
    y = jnp.dot(rows, wo[...], preferred_element_type=F32).astype(BF16)
    y_own[...] = y

    def y_copy(o, t):
        to = (kv + o) % n_kv
        to_tp = (tp + t) % n_tp
        return pltpu.make_async_remote_copy(
            src_ref=y_own, dst_ref=y_all.at[g], send_sem=y_s.at[to * n_tp + to_tp], recv_sem=y_r.at[g],
            device_id=(dp, to, to_tp), device_id_type=MESH)

    for o in far_first + [0]:
        for t in range(n_tp):
            if o or t:
                y_copy(o, t).start()
    y_all[g] = y
    for o in range(1, n_kv):
        for t in range(n_tp):
            tok_wait(((kv + o) % n_kv) * n_tp + (tp + t) % n_tp)

    def y_wait(src):
        pltpu.make_async_remote_copy(
            src_ref=y_own, dst_ref=y_all.at[src], send_sem=y_s.at[0], recv_sem=y_r.at[src],
            device_id=peer_of(1)[1], device_id_type=MESH).wait_recv()

    def up_step(i, square_sum):
        j, span_rows = up_rows(i)
        up_copy(i).wait()
        for t in range(1, n_tp):
            y_wait(j * n_tp + (tp + t) % n_tp)

        @pl.when(i > 0)
        def _():
            y_wait(j * n_tp + tp)

        base = jnp.concatenate([tokall[j * n_tp + t].astype(F32) for t in range(n_tp)], axis=1)
        for t in range(n_tp):
            base = base + y_all[j * n_tp + t].astype(F32)
        m = base.astype(BF16).astype(F32)
        mid[j] = m
        mixed = (m * mlpg[:, span_rows]).astype(BF16)
        part = jnp.dot(mixed, wup[span_rows, :], preferred_element_type=F32)

        @pl.when(i == 0)
        def _():
            acc[...] = part

        @pl.when(i > 0)
        def _():
            acc[...] += part

        return square_sum + jnp.sum(m * m, axis=1, keepdims=True)

    square_sum = lax.fori_loop(0, n_kv, up_step, jnp.zeros((batch, 1), F32))
    scale2 = lax.rsqrt(square_sum * (1.0 / width) + norm_eps)
    up = jnp.maximum(acc[...] * scale2, 0.0)
    act[...] = (up * up).astype(BF16)
    big[5].wait()

    def dn_copy(o):
        return pltpu.make_async_remote_copy(
            src_ref=stage.at[o], dst_ref=land.at[o], send_sem=dn_s.at[o], recv_sem=dn_r.at[o],
            device_id=peer_of(o)[1], device_id_type=MESH)

    def down_step(i, carry):
        o = 1 + (i + n_all // 2 - 1) % (n_all - 1) + (i // (n_all - 1)) * (n_all - 1 - (n_all // 2 - 1))
        o = o % n_all
        other, _ = peer_of(o)
        cols = pl.ds(pl.multiple_of(other * thin, thin), thin)
        stage[o] = jnp.dot(act[...], wdn[:, cols], preferred_element_type=F32)

        @pl.when(i < n_all - 1)
        def _():
            dn_copy(o).start()

        return carry

    lax.fori_loop(0, n_all, down_step, 0)
    total = mid[kv, :, pl.ds(pl.multiple_of(tp * thin, thin), thin)] + stage[0]
    for o in range(1, n_all):
        dn_copy(o).wait_recv()
        total = total + land[o]
    otok[...] = total.astype(BF16)

    for src in mate:
        pltpu.make_async_remote_copy(
            src_ref=tok, dst_ref=tokall.at[g], send_sem=tok_s.at[src], recv_sem=tok_r.at[g],
            device_id=(dp, kv, src % n_tp), device_id_type=MESH).wait_send()
    for o in range(n_kv):
        for t in range(n_tp):
            if o:
                far_tok(o, t)[1].wait_send()
            if o or t:
                y_copy(o, t).wait_send()
        if o:
            for p in range(len(pieces)):
                rs_copy(o, p).wait_send()
            cell_copy(o).wait_send()
    for o in range(1, n_all):
        dn_copy(o).wait_send()


def hand_over(a, b, c, d, out_a, out_b, out_c, out_d, sems):
    pairs = ((b, out_b), (a, out_a), (c, out_c), (d, out_d))
    copies = [pltpu.make_async_copy(x, y, sems.at[i]) for i, (x, y) in enumerate(pairs)]
    for c in copies:
        c.start()
    for c in copies:
        c.wait()


def fits_fused(tokens, w_query, w_value, memory, w_output, w_up, w_down, n_kv, n_tp):
    own_rows, heads, dv, dqk = memory.shape
    batch, thin = tokens.shape
    span = w_query.shape[0]
    held = 2 * (2 * w_query.size + w_value.size + w_output.size + w_up.size + w_down.size)
    held += 10 * memory.size
    return (
        own_rows == 1 and batch == n_kv and heads == 8 and dqk == LANES and dv % LANES == 0
        and thin % LANES == 0 and span == n_tp * thin and n_kv >= 2 and n_tp >= 2
        and w_output.shape[1] == span and held < 52 * 2**20
    )


def fused_on_device(
    tokens, mix_gain, w_query, w_key, w_value, w_igate, w_fgate, igate_bias, fgate_bias,
    memory, normalizer, stabilizer, w_output, mlp_gain, w_up, w_down,
):
    n_kv = lax.axis_size("kv")
    n_tp = lax.axis_size("tp")
    n_all = n_kv * n_tp
    batch, thin = tokens.shape
    _, heads, dv, dqk = memory.shape
    span = w_query.shape[0]
    width = n_all * thin
    halves = dv // LANES
    groups = (3 + halves) * heads
    hidden = w_up.shape[1]
    hbm_spec = pl.BlockSpec(memory_space=pltpu.HBM)
    vmem_spec = pl.BlockSpec(memory_space=pltpu.VMEM)
    vm = pltpu.VMEM
    dma = pltpu.SemaphoreType.DMA
    scratch = [
        vm((batch, thin), BF16),
        vm((n_all, batch, thin), BF16),
        vm((1, width), F32),
        vm(w_query.shape, BF16),
        vm(w_key.shape, BF16),
        vm(w_value.shape, BF16),
        vm((w_igate.shape[1], span), BF16),
        vm((w_fgate.shape[1], span), BF16),
        vm((1, igate_bias.shape[0]), F32),
        vm((1, fgate_bias.shape[0]), F32),
        vm((heads, dv, dqk), F32),
        vm((heads * dv, dqk), BF16),
        vm((heads, dqk), F32),
        vm((1, heads), F32),
        vm(w_output.shape, BF16),
        vm((1, width), F32),
        vm(w_up.shape, BF16),
        vm(w_down.shape, BF16),
        vm((n_kv, groups, LANES), F32),
        vm((n_kv, groups, LANES), F32),
        vm((heads, dv), F32),
        vm((n_kv, heads, dv), F32),
        vm((batch, span), BF16),
        vm((n_all, batch, span), BF16),
        vm((n_kv, batch, span), F32),
        vm((batch, hidden), F32),
        vm((batch, hidden), BF16),
        vm((n_all, batch, thin), F32),
        vm((n_all, batch, thin), F32),
        dma((9,)), dma((6,)), dma((n_kv,)),
        dma((n_all,)), dma((n_all,)),
        dma((n_kv, 3)), dma((n_kv, 3)),
        dma((n_kv,)), dma((n_kv,)),
        dma((n_all,)), dma((n_all,)),
        dma((n_all,)), dma((n_all,)),
    ]
    args = (
        tokens, mix_gain.reshape(1, -1), w_query, w_key, w_value, w_igate.T, w_fgate.T,
        igate_bias.reshape(1, -1), fgate_bias.reshape(1, -1), memory, normalizer, stabilizer,
        w_output, mlp_gain.reshape(1, -1), w_up, w_down,
    )
    args = [pltpu.with_memory_space_constraint(a, pltpu.HBM) for a in args]
    results = pl.pallas_call(
        functools.partial(fused_cell, n_kv, n_tp),
        out_shape=(
            jax.ShapeDtypeStruct(tokens.shape, BF16),
            jax.ShapeDtypeStruct(memory.shape, F32),
            jax.ShapeDtypeStruct(normalizer.shape, F32),
            jax.ShapeDtypeStruct(stabilizer.shape, F32),
        ),
        in_specs=[hbm_spec] * 16,
        out_specs=(vmem_spec,) * 4,
        scratch_shapes=scratch,
        compiler_params=pltpu.CompilerParams(
            collective_id=0, has_side_effects=True, vmem_limit_bytes=52 * 2**20
        ),
        name="fused_cell",
    )(*args)
    return pl.pallas_call(
        hand_over,
        out_shape=tuple(jax.ShapeDtypeStruct(r.shape, r.dtype) for r in results),
        in_specs=[vmem_spec] * 4,
        out_specs=(hbm_spec,) * 4,
        scratch_shapes=[dma((4,))],
        compiler_params=pltpu.CompilerParams(vmem_limit_bytes=2**20),
        name="hand_over",
    )(*results)


def routed(*arrays):
    tokens, w_query, w_value, memory = arrays[0], arrays[2], arrays[4], arrays[9]
    w_output, w_up, w_down = arrays[12], arrays[14], arrays[15]
    n_kv, n_tp = lax.axis_size("kv"), lax.axis_size("tp")
    if fits_fused(tokens, w_query, w_value, memory, w_output, w_up, w_down, n_kv, n_tp):
        return fused_on_device(*arrays)
    return on_device(*arrays)


def solution(mesh):
    in_specs = (
        P("dp", ("kv", "tp")),
        P(),
        P("kv", "tp"),
        P("kv", "tp"),
        P("kv", "tp"),
        P(),
        P(),
        P(),
        P(),
        P(("dp", "kv"), "tp", None, None),
        P(("dp", "kv"), "tp", None),
        P(("dp", "kv"), "tp"),
        P("tp", "kv"),
        P(),
        P(None, ("kv", "tp")),
        P(("kv", "tp"), None),
    )
    out_specs = (
        P("dp", ("kv", "tp")),
        P(("dp", "kv"), "tp", None, None),
        P(("dp", "kv"), "tp", None),
        P(("dp", "kv"), "tp"),
    )
    return jax.shard_map(
        routed, mesh=mesh, in_specs=in_specs, out_specs=out_specs, check_vma=False
    )
```

```python
import functools

import jax
import jax.numpy as jnp
from jax import lax
from jax.experimental import pallas as pl
from jax.experimental.pallas import tpu as pltpu
from jax.sharding import PartitionSpec as P

MESH = pl.DeviceIdType.MESH
F32 = jnp.float32
BF16 = jnp.bfloat16
LANES = 128


norm_eps = 1e-06


def rms_normed(rows, gain):
    wide_rows = rows.astype(jnp.float32)
    scale = lax.rsqrt(jnp.mean(wide_rows * wide_rows, axis=-1, keepdims=True) + norm_eps)
    return (wide_rows * scale * gain).astype(jnp.bfloat16)


def on_device(
    tokens,
    mix_gain,
    w_query,
    w_key,
    w_value,
    w_igate,
    w_fgate,
    igate_bias,
    fgate_bias,
    memory,
    normalizer,
    stabilizer,
    w_output,
    mlp_gain,
    w_up,
    w_down,
):
    DV, DQK = memory.shape[2:]
    kv_count = lax.axis_size("kv")
    tp_count = lax.axis_size("tp")
    kv_index = lax.axis_index("kv")
    tp_index = lax.axis_index("tp")
    own_rows = memory.shape[0]
    head_count = memory.shape[1]
    whole_rows = lax.all_gather(tokens, ("kv", "tp"), axis=1, tiled=True)
    batch_rows = whole_rows.shape[0]
    wide_rows = whole_rows.astype(jnp.float32)
    normed = rms_normed(whole_rows, mix_gain)
    row_span = w_query.shape[0]
    own_cols = lax.dynamic_slice_in_dim(normed, kv_index * row_span, row_span, 1)
    joined = lax.psum_scatter(
        jnp.concatenate(
            [
                jnp.dot(own_cols, w_query, preferred_element_type=jnp.float32),
                jnp.dot(own_cols, w_key, preferred_element_type=jnp.float32),
                jnp.dot(own_cols, w_value, preferred_element_type=jnp.float32),
            ],
            axis=1,
        ),
        "kv",
        scatter_dimension=0,
        tiled=True,
    )
    query_cols = w_query.shape[1]
    queries = joined[:, :query_cols].reshape(own_rows, head_count, DQK) * DQK ** (-0.5)
    key_rows = joined[:, query_cols : 2 * query_cols].reshape(own_rows, head_count, DQK)
    values = joined[:, 2 * query_cols :].reshape(own_rows, head_count, DV)
    own_normed = lax.dynamic_slice_in_dim(normed, kv_index * own_rows, own_rows, 0)
    igate_cols = lax.dynamic_slice_in_dim(w_igate, tp_index * head_count, head_count, 1)
    fgate_cols = lax.dynamic_slice_in_dim(w_fgate, tp_index * head_count, head_count, 1)
    ibias_own = lax.dynamic_slice_in_dim(igate_bias, tp_index * head_count, head_count, 0)
    fbias_own = lax.dynamic_slice_in_dim(fgate_bias, tp_index * head_count, head_count, 0)
    input_gate = jnp.dot(own_normed, igate_cols, preferred_element_type=jnp.float32) + ibias_own
    log_forget = jax.nn.log_sigmoid(
        jnp.dot(own_normed, fgate_cols, preferred_element_type=jnp.float32) + fbias_own
    )
    carried = log_forget + stabilizer
    new_stabilizer = jnp.maximum(carried, input_gate)
    keep_weight = jnp.exp(carried - new_stabilizer)
    fresh_weight = jnp.exp(input_gate - new_stabilizer)
    recall = jnp.einsum("bhvd,bhd->bhv", memory, queries, precision=lax.Precision.HIGHEST)
    match_score = jnp.sum(queries * key_rows, axis=-1)
    numerator = keep_weight[..., None] * recall + (fresh_weight * match_score)[..., None] * values
    denominator = keep_weight * jnp.sum(normalizer * queries, axis=-1) + fresh_weight * match_score
    floor_value = jnp.maximum(jnp.abs(denominator), jnp.exp(-new_stabilizer))
    cell_out = (
        (numerator / floor_value[..., None]).astype(jnp.bfloat16).reshape(own_rows, head_count * DV)
    )
    new_memory = (
        keep_weight[..., None, None] * memory
        + fresh_weight[..., None, None] * values[..., :, None] * key_rows[..., None, :]
    )
    new_normalizer = keep_weight[..., None] * normalizer + fresh_weight[..., None] * key_rows
    partial_value = jnp.dot(
        lax.all_gather(cell_out, "kv", axis=0, tiled=True),
        w_output,
        preferred_element_type=jnp.float32,
    )
    block_cols = partial_value.shape[1]
    pieces = lax.all_gather(
        partial_value.astype(jnp.bfloat16)[:, None, :], ("kv", "tp"), axis=1, tiled=True
    )
    summed = jnp.sum(
        pieces.astype(jnp.float32).reshape(batch_rows, kv_count, tp_count, block_cols), axis=2
    )
    middle = (wide_rows + summed.reshape(batch_rows, kv_count * block_cols)).astype(jnp.bfloat16)
    mixer_in = rms_normed(middle, mlp_gain)
    up_rows = jnp.dot(mixer_in, w_up, preferred_element_type=jnp.float32)
    activation = jnp.square(jax.nn.relu(up_rows)).astype(jnp.bfloat16)
    thin_cols = tokens.shape[1]
    down_cols = lax.psum_scatter(
        lax.dot_general(
            w_down, activation, (((0,), (1,)), ((), ())), preferred_element_type=jnp.float32
        ),
        ("kv", "tp"),
        scatter_dimension=0,
        tiled=True,
    )
    middle_own = lax.dynamic_slice_in_dim(
        middle, (kv_index * tp_count + tp_index) * thin_cols, thin_cols, 1
    )
    new_tokens = (middle_own.astype(jnp.float32) + down_cols.T).astype(jnp.bfloat16)
    return (new_tokens, new_memory, new_normalizer, new_stabilizer)


def fused_cell(
    n_kv,
    n_tp,
    tok_h, mixg_h, wq_h, wk_h, wv_h, wig_h, wfg_h, ib_h, fb_h,
    mem_h, nrm_h, stb_h, wo_h, mlpg_h, wup_h, wdn_h,
    otok, newmem, onrm, ostb,
    tok, tokall, mixg, wq, wk, wv, wig, wfg, ib, fb,
    mem, membf, nrm, stb, wo, mlpg, wup, wdn,
    snd, rcv, cell_own, cell_all, y_own, y_all, mid, act, stage, land,
    small_sem, w_sem, up_sem,
    tok_s, tok_r, rs_s, rs_r, cell_s, cell_r, y_s, y_r, dn_s, dn_r,
):
    dp = lax.axis_index("dp")
    kv = lax.axis_index("kv")
    tp = lax.axis_index("tp")
    n_all = n_kv * n_tp
    g = kv * n_tp + tp
    batch, thin = tok.shape
    span = wq.shape[0]
    heads, dv, dqk = mem.shape
    width = tokall.shape[0] * thin
    halves = dv // LANES

    def peer_of(offset):
        other = (g + offset) % n_all
        return other, (dp, other // n_tp, other % n_tp)

    barrier = pltpu.get_barrier_semaphore()
    for o in range(1, n_all):
        pl.semaphore_signal(barrier, inc=1, device_id=peer_of(o)[1], device_id_type=MESH)

    own_span = pl.ds(pl.multiple_of(kv * span, span), span)
    smalls = [
        (tok_h, tok), (mixg_h, mixg), (wig_h.at[:, own_span], wig), (wfg_h.at[:, own_span], wfg),
        (ib_h, ib), (fb_h, fb), (nrm_h.at[0], nrm), (stb_h, stb), (mlpg_h, mlpg),
    ]
    small = [pltpu.make_async_copy(a, b, small_sem.at[i]) for i, (a, b) in enumerate(smalls)]
    bigs = [(wq_h, wq), (wk_h, wk), (wv_h, wv), (mem_h.at[0], mem), (wo_h, wo), (wdn_h, wdn)]
    big = [pltpu.make_async_copy(a, b, w_sem.at[i]) for i, (a, b) in enumerate(bigs)]
    for c in small:
        c.start()
    for c in big[:5]:
        c.start()

    def up_rows(i):
        if n_kv == 4:
            far_side = kv // 2
            near = kv + far_side * (3 - 2 * kv)
            step = (i + near) % 2 if i < 2 else i
            j = 3 * far_side + (1 - 2 * far_side) * step
        else:
            j = (kv + i) % n_kv
        return j, pl.ds(pl.multiple_of(j * span, span), span)

    def up_copy(i):
        j, rows = up_rows(i)
        return pltpu.make_async_copy(wup_h.at[rows], wup.at[rows], up_sem.at[j])

    small[0].wait()
    pl.semaphore_wait(barrier, n_all - 1)

    def tok_copy(o):
        return pltpu.make_async_remote_copy(
            src_ref=tok, dst_ref=tokall.at[g], send_sem=tok_s.at[o], recv_sem=tok_r.at[g],
            device_id=peer_of(o)[1], device_id_type=MESH)

    def tok_wait(src):
        pltpu.make_async_remote_copy(
            src_ref=tok, dst_ref=tokall.at[src], send_sem=tok_s.at[0], recv_sem=tok_r.at[src],
            device_id=peer_of(1)[1], device_id_type=MESH).wait_recv()

    mate = [(kv * n_tp + (tp + t) % n_tp) for t in range(1, n_tp)]
    for src in mate:
        pltpu.make_async_remote_copy(
            src_ref=tok, dst_ref=tokall.at[g], send_sem=tok_s.at[src], recv_sem=tok_r.at[g],
            device_id=(dp, kv, src % n_tp), device_id_type=MESH).start()
    tokall[g] = tok[...]

    def far_tok(o, t):
        to = (kv + o) % n_kv
        other = to * n_tp + (tp + t) % n_tp
        return other, pltpu.make_async_remote_copy(
            src_ref=tok, dst_ref=tokall.at[g], send_sem=tok_s.at[other], recv_sem=tok_r.at[g],
            device_id=(dp, to, (tp + t) % n_tp), device_id_type=MESH)

    for o in range(1, n_kv):
        for t in range(n_tp):
            far_tok(o, t)[1].start()

    snd[:, heads : 2 * heads, :] = jnp.zeros((n_kv, heads, LANES), F32)
    for c in small[1:]:
        c.wait()

    def chunk(t):
        cols = pl.ds(pl.multiple_of((kv * n_tp + t) * thin, thin), thin)
        raw = tokall[kv * n_tp + t].astype(F32)
        return (raw * mixg[:, cols]).astype(BF16), jnp.sum(raw * raw, axis=1, keepdims=True)

    def product(x, t, w):
        rows = pl.ds(pl.multiple_of(t * thin, thin), thin)
        return jnp.dot(x, w[rows, :], preferred_element_type=F32)

    x_own, squares = chunk(tp)
    for c in big[:3]:
        c.wait()
    for i in range(n_kv):
        up_copy(i).start()
    big[5].start()
    own_parts = [product(x_own, tp, w) for w in (wq, wk, wv)]
    for src in mate:
        tok_wait(src)
    others = [((tp + t) % n_tp, chunk((tp + t) % n_tp)) for t in range(1, n_tp)]
    for _, (_, more) in others:
        squares = squares + more

    def finished(n, w):
        total = own_parts[n]
        for t, (x_t, _) in others:
            total = total + product(x_t, t, w)
        return total

    x = jnp.concatenate([chunk(t)[0] for t in range(n_tp)], axis=1)
    snd[:, heads + 2, :] = jnp.broadcast_to(squares, (n_kv, LANES))
    gate_count = wig.shape[0]
    last = (((1,), (1,)), ((), ()))
    snd[:, heads, :gate_count] = lax.dot_general(x, wig[...], last, preferred_element_type=F32)
    snd[:, heads + 1, :gate_count] = lax.dot_general(x, wfg[...], last, preferred_element_type=F32)

    pieces = [(0, 2 * heads), (2 * heads, heads), (3 * heads, halves * heads)]

    def rs_copy(o, p):
        first, size = pieces[p]
        to = (kv + o) % n_kv
        return pltpu.make_async_remote_copy(
            src_ref=snd.at[to, pl.ds(first, size)],
            dst_ref=rcv.at[o, pl.ds(first, size)],
            send_sem=rs_s.at[o, p], recv_sem=rs_r.at[o, p],
            device_id=(dp, to, tp), device_id_type=MESH)

    far_first = sorted(range(1, n_kv), key=lambda o: -min(o, n_kv - o))
    q_part = finished(0, wq)
    for h in range(heads):
        snd[:, h, :] = q_part[:, h * dqk : (h + 1) * dqk]
    for o in far_first:
        rs_copy(o, 0).start()
    k_part = finished(1, wk)
    for h in range(heads):
        snd[:, 2 * heads + h, :] = k_part[:, h * dqk : (h + 1) * dqk]
    for o in far_first:
        rs_copy(o, 1).start()
    v_part = finished(2, wv)
    for h in range(heads):
        for s in range(halves):
            at = h * dv + s * LANES
            snd[:, (3 + s) * heads + h, :] = v_part[:, at : at + LANES]
    for o in far_first:
        rs_copy(o, 2).start()
    big[3].wait()
    membf[...] = mem[...].astype(BF16).reshape(heads * dv, dqk)

    lane = lax.broadcasted_iota(jnp.int32, (heads, LANES), 1)
    sub = lax.broadcasted_iota(jnp.int32, (heads, LANES), 0)
    own_head = lane == sub + tp * heads

    def column(row):
        wide = jnp.pad(row, ((0, 0), (0, LANES - row.shape[1]))) if row.shape[1] < LANES else row
        return jnp.sum(jnp.where(own_head, jnp.broadcast_to(wide, own_head.shape), 0.0), axis=1, keepdims=True)

    def joined(p):
        first, size = pieces[p]
        total = snd[kv, first : first + size, :]
        for o in range(1, n_kv):
            rs_copy(o, p).wait_recv()
            total = total + rcv[o, first : first + size, :]
        return total

    part = joined(0)
    scale = lax.rsqrt(part[heads + 2 : heads + 3] * (1.0 / width) + norm_eps)
    q = part[:heads] * scale * dqk**-0.5
    gate_i = column(part[heads : heads + 1] * scale) + column(ib[...])
    gate_f = column(part[heads + 1 : heads + 2] * scale) + column(fb[...])
    log_forget = jnp.minimum(gate_f, 0.0) - jnp.log1p(jnp.exp(-jnp.abs(gate_f)))
    stab_wide = jnp.broadcast_to(stb[...], (heads, heads))
    eye = (lax.broadcasted_iota(jnp.int32, (heads, heads), 0)
           == lax.broadcasted_iota(jnp.int32, (heads, heads), 1))
    stab = jnp.sum(jnp.where(eye, stab_wide, 0.0), axis=1, keepdims=True)
    carried = log_forget + stab
    new_stab = jnp.maximum(carried, gate_i)
    keep = jnp.exp(carried - new_stab)
    fresh = jnp.exp(gate_i - new_stab)
    ostb[...] = jnp.sum(jnp.where(eye, jnp.broadcast_to(new_stab, (heads, heads)), 0.0), axis=0, keepdims=True)
    norm_dot = jnp.sum(nrm[...] * q, axis=1, keepdims=True)
    q_hi = q.astype(BF16)
    q_lo = (q - q_hi.astype(F32)).astype(BF16)
    wide_recall = lax.dot_general(
        jnp.concatenate([q_hi, q_lo], axis=0), membf[...], (((1,), (1,)), ((), ())),
        preferred_element_type=F32)
    wide_recall = wide_recall[:heads] + wide_recall[heads:]
    row_id = lax.broadcasted_iota(jnp.int32, (heads, dv), 0)
    recall = jnp.zeros((heads, dv), F32)
    for h in range(heads):
        recall = jnp.where(row_id == h, wide_recall[:, h * dv : (h + 1) * dv], recall)
    k = joined(1) * scale
    match = jnp.sum(q * k, axis=1, keepdims=True)
    denominator = keep * norm_dot + fresh * match
    floor_value = jnp.maximum(jnp.abs(denominator), jnp.exp(-new_stab))
    v_rows = joined(2)
    v = jnp.concatenate([v_rows[s * heads : (s + 1) * heads] * scale for s in range(halves)], axis=1)
    cell = (keep * recall + (fresh * match) * v) / floor_value
    cell = cell.astype(BF16)
    cell_own[...] = cell

    def cell_copy(o):
        to = (kv + o) % n_kv
        return pltpu.make_async_remote_copy(
            src_ref=cell_own, dst_ref=cell_all.at[kv], send_sem=cell_s.at[o], recv_sem=cell_r.at[o],
            device_id=(dp, to, tp), device_id_type=MESH)

    for o in far_first:
        cell_copy(o).start()
    cell_all[kv] = cell
    onrm[0] = keep * nrm[...] + fresh * k
    fresh_v = fresh * v
    fresh_vt = fresh_v.T
    for h in range(heads):
        newmem[0, h] = keep[h : h + 1] * mem[h] + fresh_vt[:, h : h + 1] * k[h : h + 1]
    big[4].wait()
    for o in range(1, n_kv):
        src = (kv + n_kv - o) % n_kv
        pltpu.make_async_remote_copy(
            src_ref=cell_own, dst_ref=cell_all.at[src], send_sem=cell_s.at[o], recv_sem=cell_r.at[o],
            device_id=(dp, src, tp), device_id_type=MESH).wait_recv()
    cells = cell_all[...].astype(F32)
    rows = jnp.concatenate([cells[:, h, :] for h in range(heads)], axis=1).astype(BF16)
    y = jnp.dot(rows, wo[...], preferred_element_type=F32).astype(BF16)
    y_own[...] = y

    def y_copy(o, t):
        to = (kv + o) % n_kv
        to_tp = (tp + t) % n_tp
        return pltpu.make_async_remote_copy(
            src_ref=y_own, dst_ref=y_all.at[g], send_sem=y_s.at[to * n_tp + to_tp], recv_sem=y_r.at[g],
            device_id=(dp, to, to_tp), device_id_type=MESH)

    for o in far_first + [0]:
        for t in range(n_tp):
            if o or t:
                y_copy(o, t).start()
    y_all[g] = y
    for o in range(1, n_kv):
        for t in range(n_tp):
            tok_wait(((kv + o) % n_kv) * n_tp + (tp + t) % n_tp)

    def y_wait(src):
        pltpu.make_async_remote_copy(
            src_ref=y_own, dst_ref=y_all.at[src], send_sem=y_s.at[0], recv_sem=y_r.at[src],
            device_id=peer_of(1)[1], device_id_type=MESH).wait_recv()

    def up_step(i, square_sum, total_up):
        j, span_rows = up_rows(i)
        up_copy(i).wait()
        for t in range(1, n_tp):
            y_wait(j * n_tp + (tp + t) % n_tp)

        if i > 0:
            y_wait(j * n_tp + tp)

        base = jnp.concatenate([tokall[j * n_tp + t].astype(F32) for t in range(n_tp)], axis=1)
        for t in range(n_tp):
            base = base + y_all[j * n_tp + t].astype(F32)
        m = base.astype(BF16).astype(F32)
        mid[j] = m
        mixed = (m * mlpg[:, span_rows]).astype(BF16)
        part = jnp.dot(mixed, wup[span_rows, :], preferred_element_type=F32)

        total_up = part if total_up is None else total_up + part
        return square_sum + jnp.sum(m * m, axis=1, keepdims=True), total_up

    square_sum = jnp.zeros((batch, 1), F32)
    total_up = None
    for i in range(n_kv):
        square_sum, total_up = up_step(i, square_sum, total_up)
    scale2 = lax.rsqrt(square_sum * (1.0 / width) + norm_eps)
    up = jnp.maximum(total_up * scale2, 0.0)
    act[...] = (up * up).astype(BF16)
    big[5].wait()

    def dn_copy(to, src):
        return pltpu.make_async_remote_copy(
            src_ref=stage.at[to], dst_ref=land.at[src], send_sem=dn_s.at[to], recv_sem=dn_r.at[src],
            device_id=(dp, to // n_tp, to % n_tp), device_id_type=MESH)

    targets = [
        up_rows(i)[0] * n_tp + (tp + t) % n_tp
        for i in reversed(range(n_kv)) for t in reversed(range(n_tp))
    ]
    for to in targets[:-1]:
        cols = pl.ds(pl.multiple_of(to * thin, thin), thin)
        stage[to] = jnp.dot(act[...], wdn[:, cols], preferred_element_type=F32)
        dn_copy(to, g).start()
    own_cols = pl.ds(pl.multiple_of(g * thin, thin), thin)
    total = jnp.dot(act[...], wdn[:, own_cols], preferred_element_type=F32)
    total = total + mid[kv, :, pl.ds(pl.multiple_of(tp * thin, thin), thin)]
    for src in reversed(targets[:-1]):
        dn_copy(src, src).wait_recv()
        total = total + land[src]
    otok[...] = total.astype(BF16)

    for src in mate:
        pltpu.make_async_remote_copy(
            src_ref=tok, dst_ref=tokall.at[g], send_sem=tok_s.at[src], recv_sem=tok_r.at[g],
            device_id=(dp, kv, src % n_tp), device_id_type=MESH).wait_send()
    for o in range(n_kv):
        for t in range(n_tp):
            if o:
                far_tok(o, t)[1].wait_send()
            if o or t:
                y_copy(o, t).wait_send()
        if o:
            for p in range(len(pieces)):
                rs_copy(o, p).wait_send()
            cell_copy(o).wait_send()
    for to in targets[:-1]:
        dn_copy(to, g).wait_send()


def hand_over(a, b, c, d, out_a, out_b, out_c, out_d, sems):
    pairs = ((b, out_b), (a, out_a), (c, out_c), (d, out_d))
    copies = [pltpu.make_async_copy(x, y, sems.at[i]) for i, (x, y) in enumerate(pairs)]
    for c in copies:
        c.start()
    for c in copies:
        c.wait()


def fits_fused(tokens, w_query, w_value, memory, w_output, w_up, w_down, n_kv, n_tp):
    own_rows, heads, dv, dqk = memory.shape
    batch, thin = tokens.shape
    span = w_query.shape[0]
    held = 2 * (2 * w_query.size + w_value.size + w_output.size + w_up.size + w_down.size)
    held += 10 * memory.size
    return (
        own_rows == 1 and batch == n_kv and heads == 8 and dqk == LANES and dv % LANES == 0
        and thin % LANES == 0 and span == n_tp * thin and n_kv >= 2 and n_tp >= 2
        and w_output.shape[1] == span and held < 52 * 2**20
    )


def fused_on_device(
    tokens, mix_gain, w_query, w_key, w_value, w_igate, w_fgate, igate_bias, fgate_bias,
    memory, normalizer, stabilizer, w_output, mlp_gain, w_up, w_down,
):
    n_kv = lax.axis_size("kv")
    n_tp = lax.axis_size("tp")
    n_all = n_kv * n_tp
    batch, thin = tokens.shape
    _, heads, dv, dqk = memory.shape
    span = w_query.shape[0]
    width = n_all * thin
    halves = dv // LANES
    groups = (3 + halves) * heads
    hidden = w_up.shape[1]
    hbm_spec = pl.BlockSpec(memory_space=pltpu.HBM)
    vmem_spec = pl.BlockSpec(memory_space=pltpu.VMEM)
    vm = pltpu.VMEM
    dma = pltpu.SemaphoreType.DMA
    scratch = [
        vm((batch, thin), BF16),
        vm((n_all, batch, thin), BF16),
        vm((1, width), F32),
        vm(w_query.shape, BF16),
        vm(w_key.shape, BF16),
        vm(w_value.shape, BF16),
        vm((w_igate.shape[1], span), BF16),
        vm((w_fgate.shape[1], span), BF16),
        vm((1, igate_bias.shape[0]), F32),
        vm((1, fgate_bias.shape[0]), F32),
        vm((heads, dv, dqk), F32),
        vm((heads * dv, dqk), BF16),
        vm((heads, dqk), F32),
        vm((1, heads), F32),
        vm(w_output.shape, BF16),
        vm((1, width), F32),
        vm(w_up.shape, BF16),
        vm(w_down.shape, BF16),
        vm((n_kv, groups, LANES), F32),
        vm((n_kv, groups, LANES), F32),
        vm((heads, dv), BF16),
        vm((n_kv, heads, dv), BF16),
        vm((batch, span), BF16),
        vm((n_all, batch, span), BF16),
        vm((n_kv, batch, span), F32),
        vm((batch, hidden), BF16),
        vm((n_all, batch, thin), F32),
        vm((n_all, batch, thin), F32),
        dma((9,)), dma((6,)), dma((n_kv,)),
        dma((n_all,)), dma((n_all,)),
        dma((n_kv, 3)), dma((n_kv, 3)),
        dma((n_kv,)), dma((n_kv,)),
        dma((n_all,)), dma((n_all,)),
        dma((n_all,)), dma((n_all,)),
    ]
    args = (
        tokens, mix_gain.reshape(1, -1), w_query, w_key, w_value, w_igate.T, w_fgate.T,
        igate_bias.reshape(1, -1), fgate_bias.reshape(1, -1), memory, normalizer, stabilizer,
        w_output, mlp_gain.reshape(1, -1), w_up, w_down,
    )
    args = [pltpu.with_memory_space_constraint(a, pltpu.HBM) for a in args]
    results = pl.pallas_call(
        functools.partial(fused_cell, n_kv, n_tp),
        out_shape=(
            jax.ShapeDtypeStruct(tokens.shape, BF16),
            jax.ShapeDtypeStruct(memory.shape, F32),
            jax.ShapeDtypeStruct(normalizer.shape, F32),
            jax.ShapeDtypeStruct(stabilizer.shape, F32),
        ),
        in_specs=[hbm_spec] * 16,
        out_specs=(vmem_spec,) * 4,
        scratch_shapes=scratch,
        compiler_params=pltpu.CompilerParams(
            collective_id=0, has_side_effects=True, vmem_limit_bytes=52 * 2**20
        ),
        name="fused_cell",
    )(*args)
    return pl.pallas_call(
        hand_over,
        out_shape=tuple(jax.ShapeDtypeStruct(r.shape, r.dtype) for r in results),
        in_specs=[vmem_spec] * 4,
        out_specs=(hbm_spec,) * 4,
        scratch_shapes=[dma((4,))],
        compiler_params=pltpu.CompilerParams(vmem_limit_bytes=2**20),
        name="hand_over",
    )(*results)


def routed(*arrays):
    tokens, w_query, w_value, memory = arrays[0], arrays[2], arrays[4], arrays[9]
    w_output, w_up, w_down = arrays[12], arrays[14], arrays[15]
    n_kv, n_tp = lax.axis_size("kv"), lax.axis_size("tp")
    if fits_fused(tokens, w_query, w_value, memory, w_output, w_up, w_down, n_kv, n_tp):
        return fused_on_device(*arrays)
    return on_device(*arrays)


def solution(mesh):
    in_specs = (
        P("dp", ("kv", "tp")),
        P(),
        P("kv", "tp"),
        P("kv", "tp"),
        P("kv", "tp"),
        P(),
        P(),
        P(),
        P(),
        P(("dp", "kv"), "tp", None, None),
        P(("dp", "kv"), "tp", None),
        P(("dp", "kv"), "tp"),
        P("tp", "kv"),
        P(),
        P(None, ("kv", "tp")),
        P(("kv", "tp"), None),
    )
    out_specs = (
        P("dp", ("kv", "tp")),
        P(("dp", "kv"), "tp", None, None),
        P(("dp", "kv"), "tp", None),
        P(("dp", "kv"), "tp"),
    )
    return jax.shard_map(
        routed, mesh=mesh, in_specs=in_specs, out_specs=out_specs, check_vma=False
    )
```
